256 devices in a mesh: sp: 16 (over y, x), tp: 16 (over z, core).
Axes of the slice: x: 4, y: 4, z: 8, core: 2. Of those that a mesh axis runs over, the one named last changes fastest.
Arguments:
- ask_preactivation_left: bfloat16 [8192, 2048], P('sp', 'tp'), may hold values from -6 to 6
- keep_preactivation_left: bfloat16 [8192, 2048], P('sp', 'tp'), may hold values from -6 to 6
- keep_bound_complement_left: float32 [2048], P('tp'), may hold values from 0 to 0.1
- ask_preactivation_right: bfloat16 [8192, 4096], P('sp', 'tp'), may hold values from -6 to 6
- keep_preactivation_right: bfloat16 [8192, 4096], P('sp', 'tp'), may hold values from -6 to 6
- keep_bound_complement_right: float32 [4096], P('tp'), may hold values from 0 to 0.1
- payload_entries: bfloat16 [8192, 2048], P('sp', 'tp'), may hold values from -6 to 6
- emission_switch_logits: bfloat16 [8192, 2048], P('sp', 'tp'), may hold values from -6 to 6
- added_log_keep_bias: float32 [8192, 32], P('sp', 'tp'), may hold values from -2.1 to 0
- lanewise_rescale: float32 [64], replicated, may hold values from 0.1 to 1.9
- emission_matrix_alpha: bfloat16 [1024, 2048], P('tp'), may hold values from -0.125 to 0.125
- emission_matrix_beta: bfloat16 [1024, 2048], P('tp'), may hold values from -0.125 to 0.125
- skip_stream: bfloat16 [8192, 2048], P(('sp', 'tp')), may hold values from -6 to 6
- postrecurrence_rescale: float32 [2048], replicated, may hold values from 0.1 to 1.9
- premixture_rescale: float32 [2048], replicated, may hold values from 0.1 to 1.9
- postmixture_rescale: float32 [2048], replicated, may hold values from 0.1 to 1.9
- dispatcher_columns: bfloat16 [2048, 32], P(None, 'sp'), may hold values from -0.125 to 0.125
- switch_matrix: bfloat16 [16, 2048, 4096], P('sp', None, 'tp'), may hold values from -0.125 to 0.125
- expansion_matrix: bfloat16 [16, 2048, 4096], P('sp', None, 'tp'), may hold values from -0.125 to 0.125
- contraction_matrix: bfloat16 [16, 4096, 2048], P('sp', 'tp'), may hold values from -0.125 to 0.125
- item_specialist_cluster: int32 [8192], P(('sp', 'tp')), may hold values from 0 to 15, as said below
Outputs:
- result: bfloat16 [8192, 2048], P(('sp', 'tp'))
The draws below stay inside these ranges and needn't reach their ends.
Inputs may be any that keep to these rules, and one draw needn't show every extreme that they name: `item_specialist_cluster`: in every aligned block of 32 tokens (the rows of one device) no group is named more than 3 times, and some group exactly 3 times.
All inputs are finite; a program needn't handle non-finite values.
Results may differ from the reference program's by a relative error of at most 0.023.
Values may be sent and summed in bfloat16 or wider, within the bound.
No kernel may reach another device: no remote copies, remote signals or barrier semaphores. Data moves between devices by JAX's collectives and lax.ppermute only.
A program may use at most 64 MiB of HBM per device.

```python
import jax
import jax.numpy as jnp
from jax import lax

D = 2048
HEADS_IN_SET = 16
DKA = 128
DKB = 256
DV = 64
FF = 2048
EXP_GROUP = 2
TOK_DEV = 512
BLOCK_LENGTH = 512
SEQ_STEPS = 8192
ROWS_DEV = 32
GROUPS = 16
EXPERTS = 32
CAP = 3
N_TP = 16


def forget_draw(key, columns):
    noise_part = jnp.clip(jax.random.normal(jax.random.fold_in(key, 1), (SEQ_STEPS, columns), jnp.float32), -5.0, 5.0)
    block_shift = jax.random.uniform(jax.random.fold_in(key, 2), (SEQ_STEPS // TOK_DEV, 1, 1), jnp.float32, -1.0, 1.0)
    shifted = noise_part.reshape(SEQ_STEPS // TOK_DEV, TOK_DEV, columns) + block_shift
    return shifted.reshape(SEQ_STEPS, columns).astype(jnp.bfloat16)


def draw_keep_preactivation_left(key, part):
    return forget_draw(key, HEADS_IN_SET * DKA)


def draw_keep_preactivation_right(key, part):
    return forget_draw(key, HEADS_IN_SET * DKB)


def gap_draw(key, recurrent_state_width):
    fast_share = 0.5
    fast_head = jax.random.uniform(jax.random.fold_in(key, 21), (HEADS_IN_SET, 1), jnp.float32) < fast_share
    quick_gap = jnp.exp(jax.random.uniform(jax.random.fold_in(key, 22), (HEADS_IN_SET, recurrent_state_width), jnp.float32, jnp.log(0.04), jnp.log(0.1)))
    slow_gap = jnp.exp(jax.random.uniform(jax.random.fold_in(key, 23), (HEADS_IN_SET, recurrent_state_width), jnp.float32, jnp.log(0.3 / SEQ_STEPS), jnp.log(1.5 / SEQ_STEPS)))
    return jnp.where(fast_head, quick_gap, slow_gap).reshape(HEADS_IN_SET * recurrent_state_width)


def draw_keep_bound_complement_left(key, part):
    return gap_draw(key, DKA)


def draw_keep_bound_complement_right(key, part):
    return gap_draw(key, DKB)


def draw_added_log_keep_bias(key, part):
    spike_position = jax.random.randint(jax.random.fold_in(key, 31), (3, 2 * HEADS_IN_SET), 0, SEQ_STEPS)
    spike_strength = jax.random.uniform(jax.random.fold_in(key, 32), (3, 2 * HEADS_IN_SET), jnp.float32, jnp.log(0.5), jnp.log(0.8))
    sequence_positions = jnp.arange(SEQ_STEPS, dtype=jnp.int32)[:, None]
    spike_sum = jnp.zeros((SEQ_STEPS, 2 * HEADS_IN_SET), jnp.float32)
    for selected_group in range(3):
        spike_sum = spike_sum + jnp.where(sequence_positions == spike_position[selected_group][None, :], spike_strength[selected_group][None, :], 0.0)
    return spike_sum


def draw_item_specialist_cluster(key, part):
    block_total_count = SEQ_STEPS // ROWS_DEV
    others = GROUPS - 1
    spare_rows = ROWS_DEV - CAP
    base_load = spare_rows // others
    extra_rows = spare_rows - base_load * others
    move_limit = max(0, min(CAP - base_load - 1, base_load))
    hot_group = jax.random.randint(jax.random.fold_in(key, 11), (block_total_count, 1), 0, GROUPS)
    other_index = jnp.arange(others, dtype=jnp.int32)[None, :]
    shuffled = jnp.argsort(jax.random.randint(jax.random.fold_in(key, 12), (block_total_count, others), 0, 1 << 16) * others + other_index, axis=1)
    loads = base_load + (shuffled < extra_rows).astype(jnp.int32)
    pairs = others // 2
    if pairs > 0:
        moved = jax.random.randint(jax.random.fold_in(key, 13), (block_total_count, pairs), -move_limit, move_limit + 1)
        load_shift = jnp.stack([moved, -moved], axis=2).reshape(block_total_count, 2 * pairs)
        if others > 2 * pairs:
            load_shift = jnp.concatenate([load_shift, jnp.zeros((block_total_count, 1), jnp.int32)], axis=1)
        loads = loads + load_shift
    group_index = jnp.arange(GROUPS, dtype=jnp.int32)[None, :]
    source = jnp.clip(jnp.where(group_index < hot_group, group_index, group_index - 1), 0, others - 1)
    source = jnp.broadcast_to(source, (block_total_count, GROUPS))
    all_loads = jnp.where(group_index == hot_group, CAP, jnp.take_along_axis(loads, source, axis=1))
    load_ends = jnp.cumsum(all_loads, axis=1)
    sequence_positions = jnp.arange(ROWS_DEV, dtype=jnp.int32)[None, :, None]
    group_of = jnp.sum((load_ends[:, None, :] <= sequence_positions).astype(jnp.int32), axis=2)
    row_index = jnp.arange(ROWS_DEV, dtype=jnp.int32)[None, :]
    row_order = jnp.argsort(jax.random.randint(jax.random.fold_in(key, 14), (block_total_count, ROWS_DEV), 0, 1 << 16) * ROWS_DEV + row_index, axis=1)
    group_of = jnp.take_along_axis(group_of, row_order, axis=1)
    return group_of.reshape(SEQ_STEPS).astype(jnp.int32)


def steps_of(own_key, extent, split, smallest, high):
    loudness, own = 1.0, jax.random.fold_in(own_key, 6)
    for dim, shards_of in split:
        steps = jnp.exp(jax.random.uniform(jax.random.fold_in(own, dim), (shards_of,), jnp.float32, smallest / len(split), high / len(split)))
        loudness = loudness * jnp.repeat(steps, extent[dim] // shards_of).reshape([-1 if axis == dim else 1 for axis in range(len(extent))])
    return loudness


def gaussian(rng, extent, width, bound, split=(), kind=jnp.bfloat16):
    level = steps_of(rng, extent, split, -0.22, 0.18) if split else 1.0
    drawn = jax.random.normal(rng, extent, jnp.float32) * width * level
    return jnp.minimum(jnp.maximum(drawn, -bound), bound).astype(kind)


def setup_inputs(seed: int = 0) -> dict:
    key_list = jax.random.split(jax.random.key(seed), 22)
    return {
        "ask_preactivation_left": gaussian(key_list[0], (SEQ_STEPS, HEADS_IN_SET * DKA), 1.0, 6.0, ((0, 16), (1, 16))),
        "keep_preactivation_left": draw_keep_preactivation_left(jax.random.fold_in(key_list[21], 71), 0),
        "keep_bound_complement_left": draw_keep_bound_complement_left(jax.random.fold_in(key_list[21], 71), 0),
        "ask_preactivation_right": gaussian(key_list[3], (SEQ_STEPS, HEADS_IN_SET * DKB), 1.0, 6.0, ((0, 16), (1, 16))),
        "keep_preactivation_right": draw_keep_preactivation_right(jax.random.fold_in(key_list[21], 71), 0),
        "keep_bound_complement_right": draw_keep_bound_complement_right(jax.random.fold_in(key_list[21], 71), 0),
        "payload_entries": gaussian(key_list[6], (SEQ_STEPS, 2 * HEADS_IN_SET * DV), 1.0, 6.0, ((0, 16), (1, 16))),
        "emission_switch_logits": gaussian(key_list[7], (SEQ_STEPS, 2 * HEADS_IN_SET * DV), 1.0, 6.0, ((0, 16), (1, 16))),
        "added_log_keep_bias": draw_added_log_keep_bias(jax.random.fold_in(key_list[21], 71), 0),
        "lanewise_rescale": jnp.clip(1.0 + 0.18 * jax.random.normal(key_list[9], (DV,), jnp.float32), 0.1, 1.9),
        "emission_matrix_alpha": gaussian(key_list[10], (HEADS_IN_SET * DV, D), (2 * HEADS_IN_SET * DV) ** -0.5, 0.125, ((0, 16),)),
        "emission_matrix_beta": gaussian(key_list[11], (HEADS_IN_SET * DV, D), (2 * HEADS_IN_SET * DV) ** -0.5, 0.125, ((0, 16),)),
        "skip_stream": gaussian(key_list[12], (SEQ_STEPS, D), 1.0, 6.0, ((0, 256),)),
        "postrecurrence_rescale": jnp.clip(1.0 + 0.18 * jax.random.normal(key_list[13], (D,), jnp.float32), 0.1, 1.9),
        "premixture_rescale": jnp.clip(1.0 + 0.18 * jax.random.normal(key_list[14], (D,), jnp.float32), 0.1, 1.9),
        "postmixture_rescale": jnp.clip(1.0 + 0.18 * jax.random.normal(key_list[15], (D,), jnp.float32), 0.1, 1.9),
        "dispatcher_columns": gaussian(key_list[16], (D, EXPERTS), D ** -0.5, 0.125, ((1, 16),)),
        "switch_matrix": gaussian(key_list[17], (GROUPS, D, EXP_GROUP * FF), D ** -0.5, 0.125, ((0, 16), (2, 16))),
        "expansion_matrix": gaussian(key_list[18], (GROUPS, D, EXP_GROUP * FF), D ** -0.5, 0.125, ((0, 16), (2, 16))),
        "contraction_matrix": gaussian(key_list[19], (GROUPS, EXP_GROUP * FF, D), FF ** -0.5, 0.125, ((0, 16), (1, 16))),
        "item_specialist_cluster": draw_item_specialist_cluster(jax.random.fold_in(key_list[21], 71), 0),
    }


EPSILON = 1e-06
PRECISE = lax.Precision.HIGHEST

def rms_scale(features, gain):
    return features * lax.rsqrt(lax.optimization_barrier(jnp.mean(features * features, axis=-1, keepdims=True)) + EPSILON) * gain

def block_step(carry_state, inputs):
    queries, incoming_key_rows, value_row_block, inside = inputs
    length = queries.shape[0]
    causal = lax.broadcasted_iota(jnp.int32, (length, length), 0) >= lax.broadcasted_iota(jnp.int32, (length, length), 1)
    q_decayed = queries * jnp.exp(inside)
    k_grown = incoming_key_rows * jnp.exp(-inside)
    scores = jnp.einsum('thd,shd->hts', q_decayed, k_grown, precision=PRECISE)
    scores = jnp.where(causal[None], scores, jnp.zeros_like(scores))
    outputs = jnp.einsum('hts,shv->thv', scores, value_row_block, precision=PRECISE)
    outputs = outputs + jnp.einsum('thd,hdv->thv', q_decayed, carry_state, precision=PRECISE)
    last_decay = inside[-1]
    fresh_state = jnp.einsum('shd,shv->hdv', incoming_key_rows * jnp.exp(last_decay[None] - inside), value_row_block, precision=PRECISE)
    return (jnp.exp(last_decay)[:, :, None] * carry_state + fresh_state, outputs)

def head_outputs(call_arguments):
    query_vector, forget_gate, lower_margin, spike_value, value_row_block = call_arguments
    recurrent_state_width = query_vector.shape[1]
    block_total_count = SEQ_STEPS // BLOCK_LENGTH
    block_shape = (block_total_count, BLOCK_LENGTH, 1, recurrent_state_width)
    queries = jax.nn.silu(query_vector.astype(jnp.float32)).reshape(block_shape)
    incoming_key_rows = lower_margin * jax.nn.sigmoid(-forget_gate.astype(jnp.float32)).reshape(block_shape)
    logarithm_decay = jnp.log1p(-incoming_key_rows) + spike_value.reshape(block_total_count, BLOCK_LENGTH, 1, 1)
    inside = jnp.cumsum(logarithm_decay, axis=1)
    start_state = jnp.zeros((1, recurrent_state_width, DV), jnp.float32)
    final_state, outputs = lax.scan(block_step, start_state, (queries, incoming_key_rows, value_row_block.reshape(block_total_count, BLOCK_LENGTH, 1, DV), inside))
    return outputs.reshape(SEQ_STEPS, DV)

def partitioned_result_array(query_vector, forget_gate, lower_margin, spike_value, value_row_block):
    recurrent_state_width = query_vector.shape[1] // HEADS_IN_SET
    per_head_split = (query_vector.reshape(SEQ_STEPS, HEADS_IN_SET, recurrent_state_width).transpose(1, 0, 2), forget_gate.reshape(SEQ_STEPS, HEADS_IN_SET, recurrent_state_width).transpose(1, 0, 2), lower_margin.reshape(HEADS_IN_SET, recurrent_state_width), spike_value.T, value_row_block.transpose(1, 0, 2))
    outputs = lax.map(head_outputs, per_head_split)
    return outputs.transpose(1, 0, 2)

def head_rows(outputs, gate_rows, lanewise_rescale):
    scaled = rms_scale(outputs, lanewise_rescale) * jax.nn.sigmoid(gate_rows.astype(jnp.float32))
    return scaled.astype(jnp.bfloat16).reshape(SEQ_STEPS, HEADS_IN_SET * DV)

def project(head_a, head_b, emission_matrix_alpha, emission_matrix_beta):
    slice_rows = HEADS_IN_SET * DV // N_TP
    pieces_a = head_a.reshape(SEQ_STEPS, N_TP, slice_rows)
    pieces_b = head_b.reshape(SEQ_STEPS, N_TP, slice_rows)
    weights_a = emission_matrix_alpha.reshape(N_TP, slice_rows, D)
    weights_b = emission_matrix_beta.reshape(N_TP, slice_rows, D)

    def add_slice(slice_index, running_sum):
        slice_sum = jnp.dot(pieces_a[:, slice_index], weights_a[slice_index], preferred_element_type=jnp.float32)
        slice_sum = slice_sum + jnp.dot(pieces_b[:, slice_index], weights_b[slice_index], preferred_element_type=jnp.float32)
        return running_sum + lax.optimization_barrier(slice_sum.astype(jnp.bfloat16)).astype(jnp.float32)
    return lax.fori_loop(0, N_TP, add_slice, jnp.zeros((SEQ_STEPS, D), jnp.float32))

def expert_mixture(normed, dispatcher_columns, switch_matrix, expansion_matrix, contraction_matrix, item_specialist_cluster):
    sorted_order = jnp.argsort(item_specialist_cluster, stable=True).astype(jnp.int32)
    members = item_specialist_cluster[None, :] == jnp.arange(GROUPS, dtype=jnp.int32)[:, None]
    counts = lax.optimization_barrier(jnp.sum(members.astype(jnp.int32), axis=1))
    starts = jnp.cumsum(counts) - counts
    group_slots = SEQ_STEPS // ROWS_DEV * CAP
    slice_width = EXP_GROUP * FF // N_TP

    def one_group(group):
        slot_index = jnp.arange(group_slots, dtype=jnp.int32)
        filled = slot_index < counts[group]
        token_index = sorted_order[jnp.minimum(starts[group] + slot_index, SEQ_STEPS - 1)]
        group_rows = jnp.where(filled[:, None], normed[token_index], jnp.zeros((), jnp.bfloat16))
        columns = lax.dynamic_slice_in_dim(dispatcher_columns, group * EXP_GROUP, EXP_GROUP, 1)
        scores = jax.nn.sigmoid(jnp.dot(group_rows, columns, preferred_element_type=jnp.float32))
        weights = scores / lax.optimization_barrier(jnp.sum(scores, axis=1, keepdims=True))
        gate_proj = jnp.dot(group_rows, switch_matrix[group], preferred_element_type=jnp.float32)
        up_proj = jnp.dot(group_rows, expansion_matrix[group], preferred_element_type=jnp.float32)
        hidden = (jax.nn.silu(gate_proj) * up_proj).astype(jnp.bfloat16)
        down_rows = contraction_matrix[group]

        def add_slice(slice_index, running_sum):
            first_unit = (slice_index * slice_width).astype(jnp.int32)
            hidden_part = lax.dynamic_slice_in_dim(hidden, first_unit, slice_width, 1)
            down_part = lax.dynamic_slice_in_dim(down_rows, first_unit, slice_width, 0)
            product = jnp.dot(hidden_part, down_part, preferred_element_type=jnp.float32)
            member = (first_unit // FF).astype(jnp.int32)
            member_weight = lax.dynamic_slice_in_dim(weights, member, 1, 1)
            slice_sum = member_weight * product
            return running_sum + lax.optimization_barrier(slice_sum.astype(jnp.bfloat16)).astype(jnp.float32)
        running_sum = lax.fori_loop(0, N_TP, add_slice, jnp.zeros((group_slots, D), jnp.float32))
        return (running_sum.astype(jnp.bfloat16), jnp.where(filled, token_index, SEQ_STEPS))
    routed_rows, targets = lax.map(one_group, jnp.arange(GROUPS, dtype=jnp.int32))
    empty = jnp.zeros((SEQ_STEPS, D), jnp.bfloat16)
    return empty.at[targets.reshape(-1)].set(routed_rows.reshape(-1, D), mode='drop')

def reference(ask_preactivation_left, keep_preactivation_left, keep_bound_complement_left, ask_preactivation_right, keep_preactivation_right, keep_bound_complement_right, payload_entries, emission_switch_logits, added_log_keep_bias, lanewise_rescale, emission_matrix_alpha, emission_matrix_beta, skip_stream, postrecurrence_rescale, premixture_rescale, postmixture_rescale, dispatcher_columns, switch_matrix, expansion_matrix, contraction_matrix, item_specialist_cluster):
    routing_assignment = added_log_keep_bias.reshape(SEQ_STEPS, HEADS_IN_SET, 2)
    content_coupling = payload_entries.astype(jnp.float32).reshape(SEQ_STEPS, HEADS_IN_SET, 2, DV)
    gate_pair = emission_switch_logits.reshape(SEQ_STEPS, HEADS_IN_SET, 2, DV)
    raw_leading_factor = partitioned_result_array(ask_preactivation_left, keep_preactivation_left, keep_bound_complement_left, routing_assignment[:, :, 0], content_coupling[:, :, 0])
    raw_trailing_factor = partitioned_result_array(ask_preactivation_right, keep_preactivation_right, keep_bound_complement_right, routing_assignment[:, :, 1], content_coupling[:, :, 1])
    head_a = head_rows(raw_leading_factor, gate_pair[:, :, 0], lanewise_rescale)
    head_b = head_rows(raw_trailing_factor, gate_pair[:, :, 1], lanewise_rescale)
    mixed = project(head_a, head_b, emission_matrix_alpha, emission_matrix_beta)
    h_mid = (skip_stream.astype(jnp.float32) + rms_scale(mixed, postrecurrence_rescale)).astype(jnp.bfloat16)
    normed = rms_scale(h_mid.astype(jnp.float32), premixture_rescale).astype(jnp.bfloat16)
    routed = expert_mixture(normed, dispatcher_columns, switch_matrix, expansion_matrix, contraction_matrix, item_specialist_cluster)
    return (h_mid.astype(jnp.float32) + rms_scale(routed.astype(jnp.float32), postmixture_rescale)).astype(jnp.bfloat16)
```

```python
import jax
import jax.numpy as jnp
from jax import lax
from jax.sharding import Mesh, PartitionSpec as P

EPSILON = 1e-06
F32 = jnp.float32
BF16 = jnp.bfloat16


def shifted(v, axis, by):
    n = lax.axis_size(axis)
    return lax.ppermute(v, axis, [(i, (i + by) % n) for i in range(n)])


def partner(v):
    return lax.ppermute(v, "core", [(0, 1), (1, 0)])


def dot(a, b):
    return jnp.dot(a, b, preferred_element_type=F32)


def dot_t(a, b):
    return lax.dot_general(a, b, (((1,), (1,)), ((), ())), preferred_element_type=F32)


def dot_0(a, b):
    return lax.dot_general(a, b, (((0,), (0,)), ((), ())), preferred_element_type=F32)


def rms_scale(features, gain):
    return (
        features * lax.rsqrt(jnp.mean(features * features, axis=-1, keepdims=True) + EPSILON) * gain
    )


def ring_sum(blocks):
    half = blocks[0].shape[1] // 2
    right = shifted(blocks[4][:, :half].astype(BF16), "z", 1)
    left = shifted(blocks[4][:, half:].astype(BF16), "z", -1)
    right = jnp.pad(right, ((0, 0), (0, half)))
    left = jnp.pad(left, ((0, 0), (half, 0)))
    for far in (3, 2, 1):
        right = shifted(
            (blocks[far].astype(F32) + right.astype(F32)).astype(BF16), "z", 1
        )
        left = shifted(
            (blocks[8 - far].astype(F32) + left.astype(F32)).astype(BF16), "z", -1
        )
    return blocks[0].astype(F32) + right.astype(F32) + left.astype(F32)


def pack_state(state_t, total):
    hi = total.astype(BF16)
    lo = (total - hi.astype(F32)).astype(BF16)
    rest = jnp.zeros((14, total.shape[1]), BF16)
    return jnp.concatenate([state_t.astype(BF16), hi, lo, rest], axis=0)


def unpack_state(packed):
    wide = packed.astype(F32)
    return wide[:64], wide[64:65] + wide[65:66]


def prefix_of(pieces, places, limit):
    state, total = 0.0, 0.0
    for (s_k, l_k), p_k in zip(pieces, places):
        later = 0.0
        for (_, l_m), p_m in zip(pieces, places):
            later = later + jnp.where((p_m > p_k) & (p_m < limit), l_m, 0.0)
        use = p_k < limit
        state = state + jnp.where(use, jnp.exp(later) * s_k, 0.0)
        total = total + jnp.where(use, l_k, 0.0)
    return state, total


def entering(state_t, total):
    own = pack_state(state_t, total)
    x, y = lax.axis_index("x"), lax.axis_index("y")
    row = [(state_t, total)] + [unpack_state(shifted(own, "x", k)) for k in (1, 2, 3)]
    places = [(x - k) % 4 for k in range(4)]
    whole = prefix_of(row, places, 4)
    before, before_total = prefix_of(row, places, x)
    sent = pack_state(*whole)
    rows = [unpack_state(shifted(sent, "y", k)) for k in (1, 2, 3)]
    above, _ = prefix_of(rows, [(y - k) % 4 for k in (1, 2, 3)], y)
    return jnp.exp(before_total) * above + before


def finish(raw, gate, gain):
    return (rms_scale(raw, gain) * jax.nn.sigmoid(gate.astype(F32))).astype(BF16)


def heads_of(qa, fa, gap_a, qb, fb, gap_b, values, gates, bias, gain):
    rows = qa.shape[0]
    q = jax.nn.silu(jnp.concatenate([qa, qb], axis=1).astype(F32))
    gap = jnp.concatenate([gap_a, gap_b])[None]
    key = gap * jax.nn.sigmoid(-jnp.concatenate([fa, fb], axis=1).astype(F32))
    ka = qa.shape[1]
    channel = lax.broadcasted_iota(jnp.int32, key.shape, 1)
    logf = jnp.log1p(-key) + jnp.where(channel < ka, bias[:, 0:1], bias[:, 1:2])
    at = lax.broadcasted_iota(jnp.int32, (rows, rows), 0)
    of = lax.broadcasted_iota(jnp.int32, (rows, rows), 1)
    causal = at >= of
    ones = causal.astype(BF16)
    hi = logf.astype(BF16)
    lo = (logf - hi.astype(F32)).astype(BF16)
    inside = dot(ones, hi) + dot(ones, lo)
    total = inside[-1:]
    k_last = (key * jnp.exp(total - inside)).astype(BF16)
    va, vb = values[:, :64], values[:, 64:]
    state_t = jnp.concatenate([dot_0(va, k_last[:, :ka]), dot_0(vb, k_last[:, ka:])], axis=1)
    carried = entering(state_t, total).astype(BF16)
    q_dec = (q * jnp.exp(inside)).astype(BF16)
    k_grown = (key * jnp.exp(-inside)).astype(BF16)

    def side(lanes, v, gate):
        scores = jnp.where(causal, dot_t(q_dec[:, lanes], k_grown[:, lanes]), 0.0).astype(BF16)
        raw = dot(scores, v) + dot_t(q_dec[:, lanes], carried[:, lanes])
        return finish(raw, gate, gain)

    head_a = side(slice(0, ka), va, gates[:, :64])
    head_b = side(slice(ka, None), vb, gates[:, 64:])
    return jnp.concatenate([head_a, head_b], axis=1)


def mixed_rows(heads, w_own, w_other):
    z, core = lax.axis_index("z"), lax.axis_index("core")
    parts = heads.reshape(8, 2, 32, 128)
    parts = lax.dynamic_slice_in_dim(jnp.concatenate([parts, parts], axis=0), z, 8, 0)
    keep = jnp.where(core == 0, parts[:, 0], parts[:, 1]).reshape(256, 128)
    give = jnp.where(core == 0, parts[:, 1], parts[:, 0]).reshape(256, 128)
    part = (dot(keep, w_own) + dot(partner(give), w_other)).astype(BF16)
    return ring_sum([part[32 * r : 32 * r + 32] for r in range(8)])


def expert_blocks(blocks, dispatcher, gates, ups, downs):
    rows = jnp.concatenate(blocks, axis=0)
    scores = jax.nn.sigmoid(dot(rows, dispatcher))
    member = lax.axis_index("z") // 4
    mine = jnp.where(member == 0, scores[:, 0:1], scores[:, 1:2])
    weight = mine / (scores[:, 0:1] + scores[:, 1:2])
    out = 0.0
    for g, u, d in zip(gates, ups, downs):
        hidden = (jax.nn.silu(dot(rows, g)) * dot(rows, u)).astype(BF16)
        out = out + dot(hidden, d)
    out = (out * weight).astype(BF16)
    n = blocks[0].shape[0]
    return [out[n * i : n * i + n] for i in range(len(blocks))]


def experts(chunk, dispatcher, gates, ups, downs):
    half = chunk.shape[1] // 2

    def run(blocks):
        return expert_blocks(blocks, dispatcher, gates, ups, downs)

    below = [chunk]
    above = [chunk]
    for _ in range(3):
        below.append(shifted(below[-1], "z", 1))
        above.append(shifted(above[-1], "z", -1))
    far = jnp.concatenate(
        [shifted(below[3][:, :half], "z", 1), shifted(above[3][:, half:], "z", -1)], axis=1
    )
    p0, p1, p7, p2, p6 = run([chunk, above[1], below[1], above[2], below[2]])
    p3, p5 = run([above[3], below[3]])
    (p4,) = run([far])
    return ring_sum([p0, p1, p2, p3, p4, p5, p6, p7])


def shards(
    qa, fa, gap_a, qb, fb, gap_b, values, gates, bias, gain, w_a, w_b, skip,
    post_gain, pre_gain, last_gain, dispatcher, switch, expansion, contraction, cluster,
):
    w_own = jnp.concatenate([w_a, w_b], axis=0)
    w_other = partner(w_own)
    switch, expansion, contraction = switch[0], expansion[0], contraction[0]
    others = [partner(w) for w in (switch, expansion, contraction)]
    heads = heads_of(qa, fa, gap_a, qb, fb, gap_b, values, gates, bias, gain)
    mixed = mixed_rows(heads, w_own, w_other)
    h_mid = (skip.astype(F32) + rms_scale(mixed, post_gain)).astype(BF16)
    normed = rms_scale(h_mid.astype(F32), pre_gain).astype(BF16)
    groups, capacity, count = 16, 3, skip.shape[0]
    member = cluster[:, None] == lax.broadcasted_iota(jnp.int32, (count, groups), 1)
    member = member.astype(jnp.int32)
    rank = jnp.sum(jnp.cumsum(member, axis=0) * member, axis=1) - 1
    slot = cluster * capacity + rank
    placing = (
        slot[None, :] == lax.broadcasted_iota(jnp.int32, (groups * capacity, count), 0)
    ).astype(BF16)
    sent = dot(placing, normed).astype(BF16).reshape(groups, capacity, -1)
    chunk = lax.all_to_all(sent, ("y", "x"), 0, 0, tiled=True).reshape(groups * capacity, -1)
    summed = experts(
        chunk,
        dispatcher,
        (switch, others[0]),
        (expansion, others[1]),
        (contraction, others[2]),
    ).astype(BF16)
    back = lax.all_to_all(
        summed.reshape(groups, capacity, -1), ("y", "x"), 0, 0, tiled=True
    ).reshape(groups * capacity, -1)
    routed = dot_0(placing, back)
    return (h_mid.astype(F32) + rms_scale(routed, last_gain)).astype(BF16)


def solution(mesh):
    fine = Mesh(mesh.devices.reshape(4, 4, 8, 2), ("y", "x", "z", "core"))
    sp, tp = ("y", "x"), ("z", "core")
    both = sp + tp
    placed = (
        P(sp, tp), P(sp, tp), P(tp), P(sp, tp), P(sp, tp), P(tp), P(sp, tp), P(sp, tp), P(sp, tp),
        P(), P(tp, None), P(tp, None), P(both, None), P(), P(), P(), P(None, sp),
        P(sp, None, tp), P(sp, None, tp), P(sp, tp, None), P(both),
    )
    return jax.shard_map(
        shards, mesh=fine, in_specs=placed, out_specs=P(both, None), check_vma=False
    )
```

```python
import functools

import jax
import jax.numpy as jnp
from jax import lax
from jax.experimental import pallas as pl
from jax.experimental.pallas import tpu as pltpu
from jax.sharding import Mesh, PartitionSpec as P

EPSILON = 1e-06
F32 = jnp.float32
BF16 = jnp.bfloat16
VMEM = pl.BlockSpec(memory_space=pltpu.VMEM)
SMEM = pl.BlockSpec(memory_space=pltpu.SMEM)


def shifted(v, axis, by):
    n = lax.axis_size(axis)
    return lax.ppermute(v, axis, [(i, (i + by) % n) for i in range(n)])


def partner(v):
    return lax.ppermute(v, "core", [(0, 1), (1, 0)])


def dot(a, b):
    return jnp.dot(a, b, preferred_element_type=F32)


def dot_t(a, b):
    return lax.dot_general(a, b, (((1,), (1,)), ((), ())), preferred_element_type=F32)


def dot_0(a, b):
    return lax.dot_general(a, b, (((0,), (0,)), ((), ())), preferred_element_type=F32)


def rms_scale(features, gain):
    return (
        features * lax.rsqrt(jnp.mean(features * features, axis=-1, keepdims=True) + EPSILON) * gain
    )


def call(body, outs, args, scratch=(), specs=None, flops=0, moved=0, limit=4):
    return pl.pallas_call(
        body,
        out_shape=outs,
        in_specs=specs or [VMEM] * len(args),
        out_specs=jax.tree.map(lambda _: VMEM, outs),
        scratch_shapes=list(scratch),
        cost_estimate=pl.CostEstimate(flops=flops, bytes_accessed=moved, transcendentals=0),
        compiler_params=pltpu.CompilerParams(vmem_limit_bytes=limit << 20),
    )(*args)


def half_block(rows):
    return jax.ShapeDtypeStruct((rows, 1024), BF16)


def fold_pair_body(a, b, c, d, e, f):
    e[...] = (a[...].astype(F32) + b[...].astype(F32)).astype(BF16)
    f[...] = (c[...].astype(F32) + d[...].astype(F32)).astype(BF16)


def fold_pair(one, got_one, two, got_two):
    rows = one.shape[0]
    return call(
        fold_pair_body,
        (half_block(rows), half_block(rows)),
        (one, got_one, two, got_two),
        flops=4 * rows * 1024,
        moved=12 * rows * 1024,
    )


def ring_sum(a, b):
    def right(v):
        return shifted(v, "z", 1)

    def left(v):
        return shifted(v, "z", -1)

    ra, lb = right(a[4]), left(b[4])
    rb, la = right(b[3]), left(a[5])
    for far in (3, 2, 1):
        na, nb = fold_pair(a[far], ra, b[8 - far], lb)
        ra, lb = right(na), left(nb)
        if far > 1:
            mb, ma = fold_pair(b[far - 1], rb, a[9 - far], la)
            rb, la = right(mb), left(ma)
    return ra, la, rb, lb


def ring_gather(a, b):
    def right(v):
        return shifted(v, "z", 1)

    def left(v):
        return shifted(v, "z", -1)

    as_, bs = {0: a}, {0: b}
    for k in (1, 2, 3):
        as_[-k], bs[k] = right(as_[1 - k]), left(bs[k - 1])
        bs[-k], as_[k] = right(bs[1 - k]), left(as_[k - 1])
    as_[4], bs[4] = right(as_[-3]), left(bs[3])
    order = (0, 1, 2, 3, 4, -3, -2, -1)
    return [as_[k] for k in order], [bs[k] for k in order]


def pack_state(state_t, total):
    hi = total.astype(BF16)
    lo = (total - hi.astype(F32)).astype(BF16)
    rest = jnp.zeros((14, total.shape[1]), BF16)
    return jnp.concatenate([state_t.astype(BF16), hi, lo, rest], axis=0)


def unpack_state(packed):
    wide = packed.astype(F32)
    return wide[:64], wide[64:65] + wide[65:66]


def prefix_of(pieces, places, limit):
    state, total = 0.0, 0.0
    for (s_k, l_k), p_k in zip(pieces, places):
        later = 0.0
        for (_, l_m), p_m in zip(pieces, places):
            later = later + jnp.where((p_m > p_k) & (p_m < limit), l_m, 0.0)
        use = p_k < limit
        state = state + jnp.where(use, jnp.exp(later) * s_k, 0.0)
        total = total + jnp.where(use, l_k, 0.0)
    return state, total


def entering(state_t, total):
    own = pack_state(state_t, total)
    x, y = lax.axis_index("x"), lax.axis_index("y")
    row = [(state_t, total)] + [unpack_state(shifted(own, "x", k)) for k in (1, 2, 3)]
    places = [(x - k) % 4 for k in range(4)]
    whole = prefix_of(row, places, 4)
    before, before_total = prefix_of(row, places, x)
    sent = pack_state(*whole)
    rows = [unpack_state(shifted(sent, "y", k)) for k in (1, 2, 3)]
    above, _ = prefix_of(rows, [(y - k) % 4 for k in (1, 2, 3)], y)
    return jnp.exp(before_total) * above + before


def finish(raw, gate, gain):
    return (rms_scale(raw, gain) * jax.nn.sigmoid(gate.astype(F32))).astype(BF16)


def heads_of(qa, fa, gap_a, qb, fb, gap_b, values, gates, bias, gain):
    rows = qa.shape[0]
    q = jax.nn.silu(jnp.concatenate([qa, qb], axis=1).astype(F32))
    gap = jnp.concatenate([gap_a, gap_b])[None]
    key = gap * jax.nn.sigmoid(-jnp.concatenate([fa, fb], axis=1).astype(F32))
    ka = qa.shape[1]
    channel = lax.broadcasted_iota(jnp.int32, key.shape, 1)
    logf = jnp.log1p(-key) + jnp.where(channel < ka, bias[:, 0:1], bias[:, 1:2])
    at = lax.broadcasted_iota(jnp.int32, (rows, rows), 0)
    of = lax.broadcasted_iota(jnp.int32, (rows, rows), 1)
    causal = at >= of
    ones = causal.astype(BF16)
    hi = logf.astype(BF16)
    lo = (logf - hi.astype(F32)).astype(BF16)
    inside = dot(ones, hi) + dot(ones, lo)
    total = inside[-1:]
    k_last = (key * jnp.exp(total - inside)).astype(BF16)
    va, vb = values[:, :64], values[:, 64:]
    state_t = jnp.concatenate([dot_0(va, k_last[:, :ka]), dot_0(vb, k_last[:, ka:])], axis=1)
    carried = entering(state_t, total).astype(BF16)
    q_dec = (q * jnp.exp(inside)).astype(BF16)
    k_grown = (key * jnp.exp(-inside)).astype(BF16)

    def side(lanes, v, gate):
        scores = jnp.where(causal, dot_t(q_dec[:, lanes], k_grown[:, lanes]), 0.0).astype(BF16)
        raw = dot(scores, v) + dot_t(q_dec[:, lanes], carried[:, lanes])
        return finish(raw, gate, gain)

    head_a = side(slice(0, ka), va, gates[:, :64])
    head_b = side(slice(ka, None), vb, gates[:, 64:])
    return jnp.concatenate([head_a, head_b], axis=1)


def project_body(z_ref, keep, got, w_own, w_other, *refs):
    outs, rows = refs[:16], refs[16]
    z = z_ref[0]
    for r in range(8):
        at = pl.ds(pl.multiple_of(((z + r) % 8) * 32, 32), 32)
        rows[32 * r : 32 * r + 32, :128] = keep[at, :]
        rows[32 * r : 32 * r + 32, 128:] = got[at, :]
    lhs = rows[...]
    for tile in range(4):
        cols = slice(512 * tile, 512 * tile + 512)
        part = dot(lhs[:, :128], w_own[:, cols]) + dot(lhs[:, 128:], w_other[:, cols])
        part = part.astype(BF16)
        side, first = tile // 2, 512 * (tile % 2)
        for r in range(8):
            outs[8 * side + r][:, first : first + 512] = part[32 * r : 32 * r + 32]


def mixed_parts(heads, w_own, w_other):
    core = lax.axis_index("core")
    parts = heads.reshape(8, 2, 32, 128)
    keep = jnp.where(core == 0, parts[:, 0], parts[:, 1]).reshape(256, 128)
    give = jnp.where(core == 0, parts[:, 1], parts[:, 0]).reshape(256, 128)
    outs = call(
        project_body,
        tuple(half_block(32) for _ in range(16)),
        (lax.axis_index("z")[None], keep, partner(give), w_own, w_other),
        scratch=[pltpu.VMEM((256, 256), BF16)],
        specs=[SMEM] + [VMEM] * 4,
        flops=2 * 256 * 256 * 2048,
        moved=2 << 20,
        limit=8,
    )
    a, b = outs[:8], outs[8:]
    return a[0], b[0], ring_sum(a, b)


def normed_body(a, b, ra, la, rb, lb, skip, post, pre, placing, mid, sent):
    def f(ref):
        return ref[...].astype(F32)

    left = f(a) + f(ra) + f(la)
    right = f(b) + f(rb) + f(lb)
    mixed = jnp.concatenate([left, right], axis=1)
    h = (skip[...].astype(F32) + rms_scale(mixed, post[...])).astype(BF16)
    mid[...] = h
    normed = rms_scale(h.astype(F32), pre[...]).astype(BF16)
    sent[...] = dot(placing[...], normed).astype(BF16)


def expert_body(member, *refs):
    xs, (disp, g0, g1, u0, u1, d0, d1) = refs[:16], refs[16:23]
    outs, (x, h) = refs[23:39], refs[39:]
    for r in range(8):
        x[48 * r : 48 * r + 48, :1024] = xs[r][...]
        x[48 * r : 48 * r + 48, 1024:] = xs[8 + r][...]
    rows = x[...]
    scores = jax.nn.sigmoid(dot(rows, disp[...]))
    s0, s1 = scores[:, 0:1], scores[:, 1:2]
    weight = jnp.where(member[0] == 0, s0, s1) / (s0 + s1)
    for i, (g, u) in enumerate(((g0, u0), (g1, u1))):
        gate = dot(rows, g[...])
        h[:, 256 * i : 256 * i + 256] = (jax.nn.silu(gate) * dot(rows, u[...])).astype(BF16)
    hidden = h[...]
    for tile in range(4):
        cols = slice(512 * tile, 512 * tile + 512)
        out = dot(hidden[:, :256], d0[:, cols]) + dot(hidden[:, 256:], d1[:, cols])
        out = (out * weight).astype(BF16)
        side, first = tile // 2, 512 * (tile % 2)
        for r in range(8):
            outs[8 * side + r][:, first : first + 512] = out[48 * r : 48 * r + 48]


def total_body(a, b, ra, la, rb, lb, out):
    def f(ref):
        return ref[...].astype(F32)

    out[:, :1024] = (f(a) + f(ra) + f(la)).astype(BF16)
    out[:, 1024:] = (f(b) + f(rb) + f(lb)).astype(BF16)


def experts(chunk, dispatcher, weights):
    a, b = ring_gather(chunk[:, :1024], chunk[:, 1024:])
    outs = call(
        expert_body,
        tuple(half_block(48) for _ in range(16)),
        ((lax.axis_index("z") // 4)[None], *a, *b, dispatcher, *weights),
        scratch=[pltpu.VMEM((384, 2048), BF16), pltpu.VMEM((384, 512), BF16)],
        specs=[SMEM] + [VMEM] * 23,
        flops=6 * 384 * 2048 * 512,
        moved=10 << 20,
        limit=28,
    )
    p, q = outs[:8], outs[8:]
    return call(
        total_body,
        jax.ShapeDtypeStruct((48, 2048), BF16),
        (p[0], q[0], *ring_sum(p, q)),
        flops=4 * 48 * 2048,
        moved=16 * 48 * 2048,
    )


def shards(
    qa, fa, gap_a, qb, fb, gap_b, values, gates, bias, gain, w_a, w_b, skip,
    post_gain, pre_gain, last_gain, dispatcher, switch, expansion, contraction, cluster,
):
    w_own = jnp.concatenate([w_a, w_b], axis=0)
    w_other = partner(w_own)
    own = (switch[0], expansion[0], contraction[0])
    other = [partner(w) for w in own]
    groups, capacity, count = 16, 3, skip.shape[0]
    r_of = lax.broadcasted_iota(jnp.int32, (count, count), 0)
    r_at = lax.broadcasted_iota(jnp.int32, (count, count), 1)
    same = (cluster[:, None] == cluster[None, :]) & (r_of < r_at)
    slot = cluster * capacity + jnp.sum(same.astype(jnp.int32), axis=0)
    placing = (
        slot[None, :] == lax.broadcasted_iota(jnp.int32, (groups * capacity, count), 0)
    ).astype(BF16)
    heads = heads_of(qa, fa, gap_a, qb, fb, gap_b, values, gates, bias, gain)
    a, b, ring = mixed_parts(heads, w_own, w_other)
    h_mid, sent = call(
        normed_body,
        (jax.ShapeDtypeStruct((count, 2048), BF16), jax.ShapeDtypeStruct((48, 2048), BF16)),
        (a, b, *ring, skip, post_gain[None], pre_gain[None], placing),
        flops=2 * 48 * 32 * 2048,
        moved=1 << 20,
        limit=8,
    )
    chunk = lax.all_to_all(
        sent.reshape(groups, capacity, -1), ("y", "x"), 0, 0, tiled=True
    ).reshape(groups * capacity, -1)
    summed = experts(
        chunk,
        jnp.pad(dispatcher, ((0, 0), (0, 126))),
        (own[0], other[0], own[1], other[1], own[2], other[2]),
    )
    back = lax.all_to_all(
        summed.reshape(groups, capacity, -1), ("y", "x"), 0, 0, tiled=True
    ).reshape(groups * capacity, -1)
    routed = dot_0(placing, back)
    return (h_mid.astype(F32) + rms_scale(routed, last_gain)).astype(BF16)


def solution(mesh):
    fine = Mesh(mesh.devices.reshape(4, 4, 8, 2), ("y", "x", "z", "core"))
    sp, tp = ("y", "x"), ("z", "core")
    both = sp + tp
    placed = (
        P(sp, tp), P(sp, tp), P(tp), P(sp, tp), P(sp, tp), P(tp), P(sp, tp), P(sp, tp), P(sp, tp),
        P(), P(tp, None), P(tp, None), P(both, None), P(), P(), P(), P(None, sp),
        P(sp, None, tp), P(sp, None, tp), P(sp, tp, None), P(both),
    )
    return jax.shard_map(
        shards, mesh=fine, in_specs=placed, out_specs=P(both, None), check_vma=False
    )
```

```python
import jax
import jax.numpy as jnp
from jax import lax
from jax.experimental import pallas as pl
from jax.experimental.pallas import tpu as pltpu
from jax.sharding import Mesh, PartitionSpec as P


EPSILON = 1e-06
F32 = jnp.float32
BF16 = jnp.bfloat16
VMEM = pl.BlockSpec(memory_space=pltpu.VMEM)
SMEM = pl.BlockSpec(memory_space=pltpu.SMEM)
HBM = pl.BlockSpec(memory_space=pltpu.HBM)


def shifted(v, axis, by):
    n = lax.axis_size(axis)
    return lax.ppermute(v, axis, [(i, (i + by) % n) for i in range(n)])


def partner(v):
    return lax.ppermute(v, "core", [(0, 1), (1, 0)])


def dot(a, b):
    return jnp.dot(a, b, preferred_element_type=F32)


def dot_t(a, b):
    return lax.dot_general(a, b, (((1,), (1,)), ((), ())), preferred_element_type=F32)


def dot_0(a, b):
    return lax.dot_general(a, b, (((0,), (0,)), ((), ())), preferred_element_type=F32)


def rms_scale(features, gain):
    return (
        features * lax.rsqrt(jnp.mean(features * features, axis=-1, keepdims=True) + EPSILON) * gain
    )


def call(body, outs, args, scratch=(), specs=None, flops=0, moved=0, limit=4):
    return pl.pallas_call(
        body,
        out_shape=outs,
        in_specs=specs or [VMEM] * len(args),
        out_specs=jax.tree.map(lambda _: VMEM, outs),
        scratch_shapes=list(scratch),
        cost_estimate=pl.CostEstimate(flops=flops, bytes_accessed=moved, transcendentals=0),
        compiler_params=pltpu.CompilerParams(vmem_limit_bytes=limit << 20),
    )(*args)


def neighbour(v):
    return lax.ppermute(v, "z", [(i, i ^ 1) for i in range(8)])


def from_stride(outs):
    return (outs[0], shifted(outs[1], "z", 2), shifted(outs[3], "z", -2), shifted(outs[2], "z", 4))


def ring_gather(chunk):
    below, above = [chunk], [chunk]
    for _ in range(3):
        below.append(shifted(below[-1], "z", 1))
        above.append(shifted(above[-1], "z", -1))
    far = shifted(below[3], "z", 1)
    return [*above, far, *below[:0:-1]]


def unpack(ref):
    wide = ref[...].astype(F32)
    return wide[:64], wide[64:65] + wide[65:66]


def pack(ref, lanes, state, total):
    hi = total.astype(BF16).astype(F32)
    row = lax.broadcasted_iota(jnp.int32, (16, total.shape[1]), 0)
    tail = jnp.where(row == 0, hi, jnp.where(row == 1, total - hi, 0.0))
    ref[:64, lanes] = state.astype(BF16)
    ref[64:, lanes] = tail.astype(BF16)


def prefix_of(pieces, places, limit):
    state, total = 0.0, 0.0
    for (s_k, l_k), p_k in zip(pieces, places):
        later = jnp.zeros_like(l_k)
        for (_, l_m), p_m in zip(pieces, places):
            later = later + jnp.where((p_m > p_k) & (p_m < limit), l_m, 0.0)
        use = p_k < limit
        state = state + jnp.where(use, jnp.exp(later) * s_k, 0.0)
        total = total + jnp.where(use, l_k, 0.0)
    return state, total


SIDES = (slice(0, 128), slice(128, 384))


def prepare_body(*refs):
    far, (ga, gb, bias), refs = refs[:7], refs[7:10], refs[10:]
    packed, q_dec, k_grown, weights, qa, fa, qb, fb, values, sems = refs
    near = (qa, fa, qb, fb, values, weights.at[:64], weights.at[64:])
    copies = [
        pltpu.make_async_copy(src, dst, sems.at[i]) for i, (src, dst) in enumerate(zip(far, near))
    ]
    for i in (1, 3, 4, 0, 2, 5, 6):
        copies[i].start()
    rows = qa.shape[0]
    at = lax.broadcasted_iota(jnp.int32, (rows, rows), 0)
    of = lax.broadcasted_iota(jnp.int32, (rows, rows), 1)
    ones = jnp.where(at >= of, 1.0, 0.0)
    biases = [
        jnp.sum(ones * bias[side : side + 1, :], axis=1, keepdims=True) for side in (0, 1)
    ]
    ones = ones.astype(BF16)
    copies[4].wait()
    flipped = values[...].astype(F32).T.astype(BF16)
    for side, (q, f, g, lanes) in enumerate(((qa, fa, ga, SIDES[0]), (qb, fb, gb, SIDES[1]))):
        copies[2 * side + 1].wait()
        key = g[...] * jax.nn.sigmoid(-f[...].astype(F32))
        logf = jnp.log1p(-key)
        hi = logf.astype(BF16)
        lo = (logf - hi.astype(F32)).astype(BF16)
        inside = dot(ones, hi) + dot(ones, lo) + biases[side]
        total = inside[rows - 1 : rows]
        k_last = (key * jnp.exp(total - inside)).astype(BF16)
        pack(packed, lanes, dot(flipped[64 * side : 64 * side + 64], k_last), total)
        copies[2 * side].wait()
        q_dec[:, lanes] = (jax.nn.silu(q[...].astype(F32)) * jnp.exp(inside)).astype(BF16)
        k_grown[:, lanes] = (key * jnp.exp(-inside)).astype(BF16)
    copies[5].wait()
    copies[6].wait()


def inner_body(q_dec, k_grown, values, intra):
    rows = q_dec.shape[0]
    at = lax.broadcasted_iota(jnp.int32, (rows, rows), 0)
    of = lax.broadcasted_iota(jnp.int32, (rows, rows), 1)
    for side, lanes in enumerate(SIDES):
        cols = slice(64 * side, 64 * side + 64)
        scores = jnp.where(at >= of, dot_t(q_dec[:, lanes], k_grown[:, lanes]), 0.0).astype(BF16)
        intra[:, cols] = dot(scores, values[:, cols])


def spread_body(at, own, got1, got2, got3, sent, before):
    x = at[0]
    row = [unpack(ref) for ref in (own, got1, got2, got3)]
    places = [(x + 4 - k) % 4 for k in range(4)]
    pack(sent, slice(None), *prefix_of(row, places, 4))
    state, total = prefix_of(row, places, x)
    before[:64, :] = state
    before[64:, :] = jnp.broadcast_to(total, (8, total.shape[1]))


def head_body(at, q_dec, before, got1, got2, got3, intra, gates, gain, keep, give, heads):
    y = at[3]
    rows_above = [unpack(ref) for ref in (got1, got2, got3)]
    above, _ = prefix_of(rows_above, [(y + 4 - k) % 4 for k in (1, 2, 3)], y)
    carried = (jnp.exp(before[64:65, :]) * above + before[:64, :]).astype(BF16)
    for side, lanes in enumerate(SIDES):
        cols = slice(64 * side, 64 * side + 64)
        raw = intra[:, cols] + dot_t(q_dec[:, lanes], carried[:, lanes])
        gate = jax.nn.sigmoid(gates[:, cols].astype(F32))
        heads[:, cols] = rms_scale(raw, gain[...]) * gate
    z, core = at[1], at[2]
    for out, whose in ((keep, core), (give, 1 - core)):
        for r in range(8):
            block = 2 * ((z + r) % 8) + whose
            rows = heads[pl.ds(pl.multiple_of(block * 32, 32), 32), :]
            out[32 * r : 32 * r + 32, :] = rows.astype(BF16)


def heads_of(qa, fa, gap_a, qb, fb, gap_b, values, gates, bias, gain, w_a, w_b):
    rows = qa.shape[0]
    packed_shape = jax.ShapeDtypeStruct((80, 384), BF16)
    wide = jax.ShapeDtypeStruct((rows, 384), BF16)
    far = (qa, fa, qb, fb, values, w_a, w_b)
    packed, q_dec, k_grown, w_own = call(
        prepare_body,
        (packed_shape, wide, wide, jax.ShapeDtypeStruct((128, 2048), BF16)),
        (*far, gap_a[None], gap_b[None], bias.T),
        scratch=[*(pltpu.VMEM(v.shape, BF16) for v in far[:5]), pltpu.SemaphoreType.DMA((7,))],
        specs=[HBM] * 7 + [VMEM] * 3,
        flops=6 * rows * rows * 384,
        moved=3 << 20,
        limit=60,
    )
    at = jnp.stack([lax.axis_index(name) for name in ("x", "z", "core", "y")])
    row = [shifted(packed, "x", k) for k in (1, 2, 3)]
    intra = call(
        inner_body,
        jax.ShapeDtypeStruct((rows, 128), F32),
        (q_dec, k_grown, values),
        flops=2 * rows * rows * 512,
        moved=2 << 20,
        limit=12,
    )
    sent, before = call(
        spread_body,
        (packed_shape, jax.ShapeDtypeStruct((72, 384), F32)),
        (at, packed, *row),
        specs=[SMEM] + [VMEM] * 4,
        flops=64 * 384 * 30,
        moved=400 << 10,
    )
    above = [shifted(sent, "y", k) for k in (1, 2, 3)]
    half = jax.ShapeDtypeStruct((rows // 2, 128), BF16)
    keep, give = call(
        head_body,
        (half, half),
        (at, q_dec, before, *above, intra, gates, gain[None]),
        scratch=[pltpu.VMEM((rows, 128), F32)],
        specs=[SMEM] + [VMEM] * 8,
        flops=2 * 512 * 384 * 64,
        moved=1 << 20,
        limit=8,
    )
    return keep, partner(give), w_own


def project_body(at, keep, got, near, w0, w1, w2, w3, *refs):
    outs, rows = refs[:4], refs[4]
    shift = at[0]
    for i in range(4):
        here = slice(32 * i, 32 * i + 32)
        rows[here, :128] = keep[64 * i : 64 * i + 32, :]
        rows[here, 128:256] = got[64 * i : 64 * i + 32, :]
        there = pl.ds(pl.multiple_of(((i + shift) % 4) * 32, 32), 32)
        rows[here, 256:] = near[there, :]
    for tile in range(4):
        cols = slice(512 * tile, 512 * tile + 512)
        part = dot(rows[:, :128], w0[:, cols]) + dot(rows[:, 128:256], w1[:, cols])
        part = part + dot(rows[:, 256:384], w2[:, cols]) + dot(rows[:, 384:], w3[:, cols])
        part = part.astype(BF16)
        for i in range(4):
            outs[i][:, cols] = part[32 * i : 32 * i + 32]


def odd_blocks(v, size):
    return v.reshape(4, 2, size, v.shape[1])[:, 1].reshape(4 * size, v.shape[1])


def mixed_parts(keep, got, shift, w_own, w_other, w_near):
    near = neighbour(jnp.concatenate([odd_blocks(keep, 32), odd_blocks(got, 32)], axis=1))
    outs = call(
        project_body,
        tuple(jax.ShapeDtypeStruct((32, 2048), BF16) for _ in range(4)),
        (shift, keep, got, near, w_own, w_other, w_near, partner(w_near)),
        scratch=[pltpu.VMEM((128, 512), BF16)],
        specs=[SMEM] + [VMEM] * 7,
        flops=2 * 128 * 512 * 2048,
        moved=4 << 20,
        limit=10,
    )
    return from_stride(outs)


def normed_body(p0, p1, p2, p3, skip, post, pre, placing, mid, sent):
    mixed = p0[...].astype(F32) + p1[...].astype(F32) + p2[...].astype(F32) + p3[...].astype(F32)
    h = (skip[...].astype(F32) + rms_scale(mixed, post[...])).astype(BF16)
    mid[...] = h
    normed = rms_scale(h.astype(F32), pre[...]).astype(BF16)
    sent[...] = dot(placing[...], normed).astype(BF16)


def up_rows(xs, x, g0, g1, u0, u1, hidden):
    first = 0
    for ref in xs:
        x[first : first + ref.shape[0], :] = ref[...]
        first += ref.shape[0]
    rows = x[...]
    for i, (g, u) in enumerate(((g0, u0), (g1, u1))):
        gate = dot(rows, g[...])
        hidden[:, 256 * i : 256 * i + 256] = (jax.nn.silu(gate) * dot(rows, u[...])).astype(BF16)
    return rows


def odd_body(*refs):
    up_rows(refs[:4], refs[9], *refs[4:9])


def even_body(member, *refs):
    xs, disp, (weights, hidden, weight, x) = refs[:4], refs[4], (refs[5:9], *refs[9:])
    rows = up_rows(xs, x, *weights, hidden)
    scores = jax.nn.sigmoid(dot_t(rows, disp[...]))
    s0, s1 = scores[:, 0:1], scores[:, 1:2]
    mine = jnp.where(member[0] == 0, s0, s1) / (s0 + s1)
    weight[...] = jnp.broadcast_to(mine, weight.shape)


def down_body(at, keep, near, weight, *refs):
    downs, outs, rows = refs[:4], refs[4:8], refs[8]
    shift = at[0]
    for i in range(4):
        here = slice(48 * i, 48 * i + 48)
        rows[here, :512] = keep[here, :]
        rows[here, 512:] = near[pl.ds(pl.multiple_of(((i + shift) % 4) * 48, 16), 48), :]
    scale = weight[:, 0:1]
    for tile in range(4):
        cols = slice(512 * tile, 512 * tile + 512)
        part, first = 0.0, 0
        for d in downs:
            part = part + dot(rows[:, first : first + d.shape[0]], d[:, cols])
            first += d.shape[0]
        part = (part * scale).astype(BF16)
        for i in range(4):
            outs[i][:, cols] = part[48 * i : 48 * i + 48]


def total_body(p0, p1, p2, p3, out):
    total = p0[...].astype(F32) + p1[...].astype(F32) + p2[...].astype(F32) + p3[...].astype(F32)
    out[...] = total.astype(BF16)


def experts(chunk, dispatcher, shift, ups, downs):
    own, r1, r2, r3, far, l3, l2, l1 = ring_gather(chunk)
    hidden = jax.ShapeDtypeStruct((192, 512), BF16)
    give = call(
        odd_body,
        hidden,
        (r1, r3, l3, l1, *ups),
        scratch=[pltpu.VMEM((192, 2048), BF16)],
        flops=4 * 192 * 2048 * 512,
        moved=6 << 20,
        limit=12,
    )
    near = neighbour(give)
    keep, weight = call(
        even_body,
        (hidden, jax.ShapeDtypeStruct((192, 128), F32)),
        ((lax.axis_index("z") // 4)[None], own, r2, far, l2, dispatcher, *ups),
        scratch=[pltpu.VMEM((192, 2048), BF16)],
        specs=[SMEM] + [VMEM] * 9,
        flops=4 * 192 * 2048 * 512,
        moved=6 << 20,
        limit=12,
    )
    outs = call(
        down_body,
        tuple(jax.ShapeDtypeStruct((48, 2048), BF16) for _ in range(4)),
        (shift, keep, near, weight, *downs),
        scratch=[pltpu.VMEM((192, 1024), BF16)],
        specs=[SMEM] + [VMEM] * 7,
        flops=2 * 192 * 1024 * 2048,
        moved=6 << 20,
        limit=12,
    )
    return call(
        total_body,
        jax.ShapeDtypeStruct((48, 2048), BF16),
        from_stride(outs),
        flops=4 * 48 * 2048,
        moved=16 * 48 * 2048,
    )


def shards(
    qa, fa, gap_a, qb, fb, gap_b, values, gates, bias, gain, w_a, w_b, skip,
    post_gain, pre_gain, last_gain, dispatcher, switch, expansion, contraction, cluster,
):
    switch, expansion, contraction = switch[0], expansion[0], contraction[0]
    ups = (switch, partner(switch), expansion, partner(expansion))
    shift = jnp.where(lax.axis_index("z") % 2 == 0, 3, 0)[None]
    groups, capacity, count = 16, 3, skip.shape[0]
    r_of = lax.broadcasted_iota(jnp.int32, (count, count), 0)
    r_at = lax.broadcasted_iota(jnp.int32, (count, count), 1)
    same = (cluster[:, None] == cluster[None, :]) & (r_of < r_at)
    slot = cluster * capacity + jnp.sum(same.astype(jnp.int32), axis=0)
    placing = (
        slot[None, :] == lax.broadcasted_iota(jnp.int32, (groups * capacity, count), 0)
    ).astype(BF16)
    keep, got, w_own = heads_of(
        qa, fa, gap_a, qb, fb, gap_b, values, gates, bias, gain, w_a, w_b
    )
    parts = mixed_parts(keep, got, shift, w_own, partner(w_own), neighbour(w_own))
    near_rows = neighbour(contraction)
    h_mid, sent = call(
        normed_body,
        (jax.ShapeDtypeStruct((count, 2048), BF16), jax.ShapeDtypeStruct((48, 2048), BF16)),
        (*parts, skip, post_gain[None], pre_gain[None], placing),
        flops=2 * 48 * 32 * 2048,
        moved=1 << 20,
        limit=8,
    )
    chunk = lax.all_to_all(
        sent.reshape(groups, capacity, -1), ("y", "x"), 0, 0, tiled=True
    ).reshape(groups * capacity, -1)
    downs = (contraction, partner(contraction), near_rows, partner(near_rows))
    summed = experts(chunk, dispatcher.T, shift, ups, downs)
    back = lax.all_to_all(
        summed.reshape(groups, capacity, -1), ("y", "x"), 0, 0, tiled=True
    ).reshape(groups * capacity, -1)
    routed = dot_0(placing, back)
    return (h_mid.astype(F32) + rms_scale(routed, last_gain)).astype(BF16)


def solution(mesh):
    fine = Mesh(mesh.devices.reshape(4, 4, 8, 2), ("y", "x", "z", "core"))
    sp, tp = ("y", "x"), ("z", "core")
    both = sp + tp
    placed = (
        P(sp, tp), P(sp, tp), P(tp), P(sp, tp), P(sp, tp), P(tp), P(sp, tp), P(sp, tp), P(sp, tp),
        P(), P(tp, None), P(tp, None), P(both, None), P(), P(), P(), P(None, sp),
        P(sp, None, tp), P(sp, None, tp), P(sp, tp, None), P(both),
    )

    return jax.shard_map(
        shards, mesh=fine, in_specs=placed, out_specs=P(both, None), check_vma=False
    )
```

```python
import jax
import jax.numpy as jnp
from jax import lax
from jax.experimental import pallas as pl
from jax.experimental.pallas import tpu as pltpu
from jax.sharding import Mesh, PartitionSpec as P


EPSILON = 1e-06
F32 = jnp.float32
BF16 = jnp.bfloat16
VMEM = pl.BlockSpec(memory_space=pltpu.VMEM)
SMEM = pl.BlockSpec(memory_space=pltpu.SMEM)
HBM = pl.BlockSpec(memory_space=pltpu.HBM)


def shifted(v, axis, by):
    n = lax.axis_size(axis)
    return lax.ppermute(v, axis, [(i, (i + by) % n) for i in range(n)])


def partner(v):
    return lax.ppermute(v, "core", [(0, 1), (1, 0)])


def dot(a, b):
    return jnp.dot(a, b, preferred_element_type=F32)


def dot_t(a, b):
    return lax.dot_general(a, b, (((1,), (1,)), ((), ())), preferred_element_type=F32)


def dot_0(a, b):
    return lax.dot_general(a, b, (((0,), (0,)), ((), ())), preferred_element_type=F32)


def rms_scale(features, gain):
    return (
        features * lax.rsqrt(jnp.mean(features * features, axis=-1, keepdims=True) + EPSILON) * gain
    )


def call(body, outs, args, scratch=(), specs=None, flops=0, moved=0, limit=4):
    return pl.pallas_call(
        body,
        out_shape=outs,
        in_specs=specs or [VMEM] * len(args),
        out_specs=jax.tree.map(lambda _: VMEM, outs),
        scratch_shapes=list(scratch),
        cost_estimate=pl.CostEstimate(flops=flops, bytes_accessed=moved, transcendentals=0),
        compiler_params=pltpu.CompilerParams(vmem_limit_bytes=limit << 20),
    )(*args)


def neighbour(v):
    return lax.ppermute(v, "z", [(i, i ^ 1) for i in range(8)])


def from_stride(outs):
    return (outs[0], shifted(outs[1], "z", 2), shifted(outs[3], "z", -2), shifted(outs[2], "z", 4))


def ring_gather(chunk):
    below, above = [chunk], [chunk]
    for _ in range(3):
        below.append(shifted(below[-1], "z", 1))
        above.append(shifted(above[-1], "z", -1))
    far = shifted(below[3], "z", 1)
    return [*above, far, *below[:0:-1]]


def unpack(ref):
    wide = ref[...].astype(F32)
    return wide[:64], wide[64:65] + wide[65:66]


def pack(ref, lanes, state, total):
    hi = total.astype(BF16).astype(F32)
    row = lax.broadcasted_iota(jnp.int32, (16, total.shape[1]), 0)
    tail = jnp.where(row == 0, hi, jnp.where(row == 1, total - hi, 0.0))
    ref[:64, lanes] = state.astype(BF16)
    ref[64:, lanes] = tail.astype(BF16)


def prefix_of(pieces, places, limit):
    state, total = 0.0, 0.0
    for (s_k, l_k), p_k in zip(pieces, places):
        later = jnp.zeros_like(l_k)
        for (_, l_m), p_m in zip(pieces, places):
            later = later + jnp.where((p_m > p_k) & (p_m < limit), l_m, 0.0)
        use = p_k < limit
        state = state + jnp.where(use, jnp.exp(later) * s_k, 0.0)
        total = total + jnp.where(use, l_k, 0.0)
    return state, total


SIDES = (slice(0, 128), slice(128, 384))


def prepare_body(*refs):
    far, (ga, gb, bias), refs = refs[:7], refs[7:10], refs[10:]
    packed, both, weights, qa, fa, qb, fb, values, sems = refs
    near = (qa, fa, qb, fb, values, weights.at[:64], weights.at[64:])
    copies = [
        pltpu.make_async_copy(src, dst, sems.at[i]) for i, (src, dst) in enumerate(zip(far, near))
    ]
    for i in (1, 3, 4, 0, 2, 5, 6):
        copies[i].start()
    rows = qa.shape[0]
    at = lax.broadcasted_iota(jnp.int32, (rows, rows), 0)
    of = lax.broadcasted_iota(jnp.int32, (rows, rows), 1)
    ones = jnp.where(at >= of, 1.0, 0.0)
    biases = [
        jnp.sum(ones * bias[side : side + 1, :], axis=1, keepdims=True) for side in (0, 1)
    ]
    ones = ones.astype(BF16)
    copies[4].wait()
    flipped = values[...].astype(F32).T.astype(BF16)
    for side, (q, f, g, lanes) in enumerate(((qa, fa, ga, SIDES[0]), (qb, fb, gb, SIDES[1]))):
        copies[2 * side + 1].wait()
        key = g[...] * jax.nn.sigmoid(-f[...].astype(F32))
        logf = jnp.log1p(-key)
        hi = logf.astype(BF16)
        lo = (logf - hi.astype(F32)).astype(BF16)
        inside = dot(ones, hi) + dot(ones, lo) + biases[side]
        total = inside[rows - 1 : rows]
        k_last = (key * jnp.exp(total - inside)).astype(BF16)
        pack(packed, lanes, dot(flipped[64 * side : 64 * side + 64], k_last), total)
        copies[2 * side].wait()
        both[:rows, lanes] = (jax.nn.silu(q[...].astype(F32)) * jnp.exp(inside)).astype(BF16)
        both[rows:, lanes] = (key * jnp.exp(-inside)).astype(BF16)
    copies[5].wait()
    copies[6].wait()


def inner_body(both, values, intra):
    rows = values.shape[0]
    at = lax.broadcasted_iota(jnp.int32, (rows, rows), 0)
    of = lax.broadcasted_iota(jnp.int32, (rows, rows), 1)
    for side, lanes in enumerate(SIDES):
        cols = slice(64 * side, 64 * side + 64)
        scores = jnp.where(at >= of, dot_t(both[:rows, lanes], both[rows:, lanes]), 0.0).astype(BF16)
        intra[:, cols] = dot(scores, values[:, cols])


def spread_body(at, own, got1, got2, got3, sent, before):
    x = at[0]
    row = [unpack(ref) for ref in (own, got1, got2, got3)]
    places = [(x + 4 - k) % 4 for k in range(4)]
    pack(sent, slice(None), *prefix_of(row, places, 4))
    state, total = prefix_of(row, places, x)
    before[:64, :] = state
    before[64:, :] = jnp.broadcast_to(total, (8, total.shape[1]))


def head_body(at, both, before, got1, got2, got3, intra, gates, gain, keep, give, heads):
    y = at[3]
    rows_above = [unpack(ref) for ref in (got1, got2, got3)]
    above, _ = prefix_of(rows_above, [(y + 4 - k) % 4 for k in (1, 2, 3)], y)
    carried = (jnp.exp(before[64:65, :]) * above + before[:64, :]).astype(BF16)
    for side, lanes in enumerate(SIDES):
        cols = slice(64 * side, 64 * side + 64)
        raw = intra[:, cols] + dot_t(both[:512, lanes], carried[:, lanes])
        gate = jax.nn.sigmoid(gates[:, cols].astype(F32))
        heads[:, cols] = rms_scale(raw, gain[...]) * gate
    z, core = at[1], at[2]
    for out, whose in ((keep, core), (give, 1 - core)):
        for r in range(8):
            block = 2 * ((z + r) % 8) + whose
            rows = heads[pl.ds(pl.multiple_of(block * 32, 32), 32), :]
            out[32 * r : 32 * r + 32, :] = rows.astype(BF16)


def heads_of(qa, fa, gap_a, qb, fb, gap_b, values, gates, bias, gain, w_a, w_b):
    rows = qa.shape[0]
    packed_shape = jax.ShapeDtypeStruct((80, 384), BF16)
    wide = jax.ShapeDtypeStruct((2 * rows, 384), BF16)
    far = (qa, fa, qb, fb, values, w_a, w_b)
    packed, both, w_own = call(
        prepare_body,
        (packed_shape, wide, jax.ShapeDtypeStruct((128, 2048), BF16)),
        (*far, gap_a[None], gap_b[None], bias.T),
        scratch=[*(pltpu.VMEM(v.shape, BF16) for v in far[:5]), pltpu.SemaphoreType.DMA((7,))],
        specs=[HBM] * 7 + [VMEM] * 3,
        flops=6 * rows * rows * 384,
        moved=3 << 20,
        limit=60,
    )
    at = jnp.stack([lax.axis_index(name) for name in ("x", "z", "core", "y")])
    row = [shifted(packed, "x", k) for k in (1, 2, 3)]
    intra = call(
        inner_body,
        jax.ShapeDtypeStruct((rows, 128), F32),
        (both, values),
        flops=2 * rows * rows * 512,
        moved=2 << 20,
        limit=12,
    )
    sent, before = call(
        spread_body,
        (packed_shape, jax.ShapeDtypeStruct((72, 384), F32)),
        (at, packed, *row),
        specs=[SMEM] + [VMEM] * 4,
        flops=64 * 384 * 30,
        moved=400 << 10,
    )
    above = [shifted(sent, "y", k) for k in (1, 2, 3)]
    half = jax.ShapeDtypeStruct((rows // 2, 128), BF16)
    keep, give = call(
        head_body,
        (half, half),
        (at, both, before, *above, intra, gates, gain[None]),
        scratch=[pltpu.VMEM((rows, 128), F32)],
        specs=[SMEM] + [VMEM] * 8,
        flops=2 * 512 * 384 * 64,
        moved=1 << 20,
        limit=8,
    )
    return keep, partner(give), w_own


def project_body(at, keep, got, near, w0, w1, w2, w3, *refs):
    outs, rows = refs[:4], refs[4]
    shift = at[0]
    for i in range(4):
        here = slice(32 * i, 32 * i + 32)
        rows[here, :128] = keep[64 * i : 64 * i + 32, :]
        rows[here, 128:256] = got[64 * i : 64 * i + 32, :]
        there = pl.ds(pl.multiple_of(((i + shift) % 4) * 32, 32), 32)
        rows[here, 256:] = near[there, :]
    for tile in range(4):
        cols = slice(512 * tile, 512 * tile + 512)
        part = dot(rows[:, :128], w0[:, cols]) + dot(rows[:, 128:256], w1[:, cols])
        part = part + dot(rows[:, 256:384], w2[:, cols]) + dot(rows[:, 384:], w3[:, cols])
        part = part.astype(BF16)
        for i in range(4):
            outs[i][:, cols] = part[32 * i : 32 * i + 32]


def odd_blocks(v, size):
    return v.reshape(4, 2, size, v.shape[1])[:, 1].reshape(4 * size, v.shape[1])


def mixed_parts(keep, got, shift, w_own, w_other, w_near):
    near = neighbour(jnp.concatenate([odd_blocks(keep, 32), odd_blocks(got, 32)], axis=1))
    outs = call(
        project_body,
        tuple(jax.ShapeDtypeStruct((32, 2048), BF16) for _ in range(4)),
        (shift, keep, got, near, w_own, w_other, w_near, partner(w_near)),
        scratch=[pltpu.VMEM((128, 512), BF16)],
        specs=[SMEM] + [VMEM] * 7,
        flops=2 * 128 * 512 * 2048,
        moved=4 << 20,
        limit=10,
    )
    return from_stride(outs)


def normed_body(p0, p1, p2, p3, skip, post, pre, placing, mid, sent):
    mixed = p0[...].astype(F32) + p1[...].astype(F32) + p2[...].astype(F32) + p3[...].astype(F32)
    h = (skip[...].astype(F32) + rms_scale(mixed, post[...])).astype(BF16)
    mid[...] = h
    normed = rms_scale(h.astype(F32), pre[...]).astype(BF16)
    sent[...] = dot(placing[...], normed).astype(BF16)


def up_rows(xs, x, g0, g1, u0, u1, hidden):
    for i, (ref, first) in enumerate(xs):
        x[48 * i : 48 * i + 48, :] = ref[first : first + 48, :]
    rows = x[...]
    for i, (g, u) in enumerate(((g0, u0), (g1, u1))):
        gate = dot(rows, g[...])
        hidden[:, 256 * i : 256 * i + 256] = (jax.nn.silu(gate) * dot(rows, u[...])).astype(BF16)
    return rows


def odd_body(*refs):
    odd, even, ups, (hidden, early, x) = refs[:4], refs[4:7], refs[7:11], refs[11:]
    for i, ref in enumerate(even):
        early[48 * i : 48 * i + 48, :] = ref[...]
    up_rows([(odd[i], 0) for i in range(4)], x, *ups, hidden)


def even_body(member, *refs):
    early, far, disp, ups, downs = refs[0], refs[1], refs[2], refs[3:7], refs[7:9]
    part, weight, x, hidden = refs[9:]
    rows = up_rows([(early, 0), (early, 48), (far, 0), (early, 96)], x, *ups, hidden)
    scores = jax.nn.sigmoid(dot_t(rows, disp[...]))
    s0, s1 = scores[:, 0:1], scores[:, 1:2]
    mine = jnp.where(member[0] == 0, s0, s1) / (s0 + s1)
    weight[...] = jnp.broadcast_to(mine, weight.shape)
    for tile in range(4):
        cols = slice(512 * tile, 512 * tile + 512)
        out = dot(hidden[:, :256], downs[0][:, cols]) + dot(hidden[:, 256:], downs[1][:, cols])
        part[:, cols] = out.astype(BF16)


def down_body(at, part, near, weight, d0, d1, *refs):
    outs, rows = refs[:4], refs[4]
    shift = at[0]
    for i in range(4):
        there = pl.ds(pl.multiple_of(((i + shift) % 4) * 48, 16), 48)
        rows[48 * i : 48 * i + 48, :] = near[there, :]
    scale = weight[:, 0:1]
    for tile in range(4):
        cols = slice(512 * tile, 512 * tile + 512)
        out = dot(rows[:, :256], d0[:, cols]) + dot(rows[:, 256:], d1[:, cols])
        out = ((part[:, cols] + out) * scale).astype(BF16)
        for i in range(4):
            outs[i][:, cols] = out[48 * i : 48 * i + 48]


def total_body(p0, p1, p2, p3, out):
    total = p0[...].astype(F32) + p1[...].astype(F32) + p2[...].astype(F32) + p3[...].astype(F32)
    out[...] = total.astype(BF16)


def experts(chunk, dispatcher, shift, ups, downs):
    own, r1, r2, r3, far, l3, l2, l1 = ring_gather(chunk)
    hidden = jax.ShapeDtypeStruct((192, 512), BF16)
    give, early = call(
        odd_body,
        (hidden, jax.ShapeDtypeStruct((144, 2048), BF16)),
        (r1, r3, l3, l1, own, r2, l2, *ups),
        scratch=[pltpu.VMEM((192, 2048), BF16)],
        flops=4 * 192 * 2048 * 512,
        moved=6 << 20,
        limit=12,
    )
    near = neighbour(give)
    part, weight = call(
        even_body,
        (jax.ShapeDtypeStruct((192, 2048), BF16), jax.ShapeDtypeStruct((192, 128), F32)),
        ((lax.axis_index("z") // 4)[None], early, far, dispatcher, *ups, *downs[:2]),
        scratch=[pltpu.VMEM((192, 2048), BF16), pltpu.VMEM((192, 512), BF16)],
        specs=[SMEM] + [VMEM] * 9,
        flops=6 * 192 * 2048 * 512,
        moved=8 << 20,
        limit=16,
    )
    outs = call(
        down_body,
        tuple(jax.ShapeDtypeStruct((48, 2048), BF16) for _ in range(4)),
        (shift, part, near, weight, *downs[2:]),
        scratch=[pltpu.VMEM((192, 512), BF16)],
        specs=[SMEM] + [VMEM] * 5,
        flops=2 * 192 * 512 * 2048,
        moved=5 << 20,
        limit=12,
    )
    return call(
        total_body,
        jax.ShapeDtypeStruct((48, 2048), BF16),
        from_stride(outs),
        flops=4 * 48 * 2048,
        moved=16 * 48 * 2048,
    )


def shards(
    qa, fa, gap_a, qb, fb, gap_b, values, gates, bias, gain, w_a, w_b, skip,
    post_gain, pre_gain, last_gain, dispatcher, switch, expansion, contraction, cluster,
):
    switch, expansion, contraction = switch[0], expansion[0], contraction[0]
    ups = (switch, partner(switch), expansion, partner(expansion))
    shift = jnp.where(lax.axis_index("z") % 2 == 0, 3, 0)[None]
    groups, capacity, count = 16, 3, skip.shape[0]
    r_of = lax.broadcasted_iota(jnp.int32, (count, count), 0)
    r_at = lax.broadcasted_iota(jnp.int32, (count, count), 1)
    same = (cluster[:, None] == cluster[None, :]) & (r_of < r_at)
    slot = cluster * capacity + jnp.sum(same.astype(jnp.int32), axis=0)
    placing = (
        slot[None, :] == lax.broadcasted_iota(jnp.int32, (groups * capacity, count), 0)
    ).astype(BF16)
    keep, got, w_own = heads_of(
        qa, fa, gap_a, qb, fb, gap_b, values, gates, bias, gain, w_a, w_b
    )
    parts = mixed_parts(keep, got, shift, w_own, partner(w_own), neighbour(w_own))
    near_rows = neighbour(contraction)
    h_mid, sent = call(
        normed_body,
        (jax.ShapeDtypeStruct((count, 2048), BF16), jax.ShapeDtypeStruct((48, 2048), BF16)),
        (*parts, skip, post_gain[None], pre_gain[None], placing),
        flops=2 * 48 * 32 * 2048,
        moved=1 << 20,
        limit=8,
    )
    chunk = lax.all_to_all(
        sent.reshape(groups, capacity, -1), ("y", "x"), 0, 0, tiled=True
    ).reshape(groups * capacity, -1)
    downs = (contraction, partner(contraction), near_rows, partner(near_rows))
    summed = experts(chunk, dispatcher.T, shift, ups, downs)
    back = lax.all_to_all(
        summed.reshape(groups, capacity, -1), ("y", "x"), 0, 0, tiled=True
    ).reshape(groups * capacity, -1)
    routed = dot_0(placing, back)
    return (h_mid.astype(F32) + rms_scale(routed, last_gain)).astype(BF16)


def solution(mesh):
    fine = Mesh(mesh.devices.reshape(4, 4, 8, 2), ("y", "x", "z", "core"))
    sp, tp = ("y", "x"), ("z", "core")
    both = sp + tp
    placed = (
        P(sp, tp), P(sp, tp), P(tp), P(sp, tp), P(sp, tp), P(tp), P(sp, tp), P(sp, tp), P(sp, tp),
        P(), P(tp, None), P(tp, None), P(both, None), P(), P(), P(), P(None, sp),
        P(sp, None, tp), P(sp, None, tp), P(sp, tp, None), P(both),
    )

    return jax.shard_map(
        shards, mesh=fine, in_specs=placed, out_specs=P(both, None), check_vma=False
    )
```
